32 devices in a mesh: sp: 16 (over z, y, x), tp: 2 (over core).
Axes of the slice: x: 2, y: 2, z: 4, core: 2. Of those that a mesh axis runs over, the one named last changes fastest.
Arguments:
- ssm_input: bfloat16 [4096, 1024], P('sp', 'tp'), may hold values from -6 to 6
- lam_real: float32 [64, 64], P('tp'), may hold values from -0.034 to -2.197265625e-05, as said below
- lam_imag: float32 [64, 64], P('tp'), may hold values from -3 to 3, as said below
- state_in: float32 [2, 64, 16, 64], P(None, 'tp'), may hold values from -2 to 2
- read_out: float32 [64, 128, 16], P('tp'), may hold values from -0.5 to 0.5
- channel_skip: float32 [1024], P('tp'), may hold values from -3 to 3
- glu_weight: bfloat16 [1024, 1024], replicated, may hold values from -0.1875 to 0.1875
- out_weight: bfloat16 [1024, 2048], replicated, may hold values from -0.375 to 0.375
- residual: bfloat16 [4096, 2048], P(('sp', 'tp')), may hold values from -6 to 6
- norm_gain: float32 [2048], replicated, may hold values from 0.1 to 1.9
- expert_ids: int32 [4096, 2], P(('sp', 'tp')), may hold values from 0 to 31, as said below
- route_weight: float32 [4096, 2], P(('sp', 'tp')), may hold values from 0.25 to 1
- expert_gate: bfloat16 [32, 2048, 512], P(('sp', 'tp')), may hold values from -0.125 to 0.125
- expert_up: bfloat16 [32, 2048, 512], P(('sp', 'tp')), may hold values from -0.125 to 0.125
- expert_down: bfloat16 [32, 512, 2048], P(('sp', 'tp')), may hold values from -0.25 to 0.25
Outputs:
- layer_out: bfloat16 [4096, 2048], P(('sp', 'tp'))
The draws below stay inside these ranges and needn't reach their ends.
Inputs may be any that keep to these rules, and one draw needn't show every extreme that they name: `lam_real`: strictly negative. `lam_imag`: magnitude at least 0.5. `expert_ids`: A token's two experts differ and lie in the same group of 8 consecutive experts. Among the 128 rows of one device (aligned blocks) no expert is named more than 16 times, and some expert exactly 16 times; every expert is named in every such block.
All inputs are finite; a program needn't handle non-finite values.
Results may differ from the reference program's by a relative error of at most 0.006.
Values may be sent and summed in bfloat16 or wider, within the bound.
A program may use at most 128 MiB of HBM per device.

```python
import jax
import jax.numpy as jnp
import numpy as np
from jax import lax

D = 2048
GROUP_CH = 16
SSMG = 64
STATE = 64
SSMW = 1024
FF = 512
GROUPS = 4
EXPERTS = 32
ROWS_SP = 256
DEV_ROWS = 128
CAP = 16
TOKENS = 4096
N_SP = 16
N_TP = 2


def ssm_modes(key):
    base = jax.random.fold_in(key, 7)
    keys = jax.random.split(base, 5)
    share = 0.5
    slow_mask = jax.random.uniform(keys[0], (SSMG, STATE), jnp.float32) < share
    slow_rate = jax.random.uniform(keys[1], (SSMG, STATE), jnp.float32, 0.1, 1.0) / TOKENS
    fast_rate = jnp.exp(jax.random.uniform(keys[2], (SSMG, STATE), jnp.float32, jnp.log(0.01), jnp.log(0.033)))
    lam_real = -jnp.where(slow_mask, slow_rate, fast_rate)
    turn = jax.random.uniform(keys[3], (SSMG, STATE), jnp.float32, 0.5, 3.0)
    signs = jnp.where(jax.random.uniform(keys[4], (SSMG, STATE), jnp.float32) < 0.5, -1.0, 1.0)
    return (lam_real, turn * signs)


def draw_lam_real(key, part):
    return ssm_modes(key)[0].astype(jnp.float32)


def draw_lam_imag(key, part):
    return ssm_modes(key)[1].astype(jnp.float32)


def draw_state_in(key, part):
    lam_real, lam_imag = ssm_modes(key)
    magnitude = jnp.exp(lam_real)
    numer_re = magnitude * jnp.cos(lam_imag) - 1.0
    numer_im = magnitude * jnp.sin(lam_imag)
    hold_size = jnp.sqrt((numer_re * numer_re + numer_im * numer_im) / (lam_real * lam_real + lam_imag * lam_imag))
    spread = jnp.sqrt((1.0 - jnp.exp(2.0 * lam_real)) / (2.0 * GROUP_CH)) / hold_size
    noise = jnp.clip(jax.random.normal(jax.random.fold_in(key, 9), (2, SSMG, GROUP_CH, STATE), jnp.float32), -4.0, 4.0)
    return (noise * spread[None, :, None, :]).astype(jnp.float32)


def draw_expert_ids(key, part):
    block_count = TOKENS // DEV_ROWS
    per_group = EXPERTS // GROUPS
    shares = np.array([DEV_ROWS // 2, DEV_ROWS // 4, DEV_ROWS // 8, DEV_ROWS // 8])
    share_of = np.repeat(np.arange(4), shares)
    starts = np.concatenate([np.zeros(1, np.int64), np.cumsum(shares)[:-1]])
    rank_in = jnp.asarray(np.arange(DEV_ROWS) - starts[share_of], jnp.int32)
    share_index = jnp.asarray(share_of, jnp.int32)
    base = jax.random.fold_in(key, 13)

    def member_order(member_key):
        return jax.random.permutation(member_key, per_group)

    def one_block(block_key):
        keys = jax.random.split(block_key, 3)
        group_order = jax.random.permutation(keys[0], GROUPS).astype(jnp.int32)
        members = jax.vmap(member_order)(jax.random.split(keys[1], GROUPS)).astype(jnp.int32)
        chosen = group_order[share_index]
        first_pick = members[chosen, 2 * rank_in % per_group]
        second_pick = members[chosen, (2 * rank_in + 1) % per_group]
        pairs = jnp.stack([chosen * per_group + first_pick, chosen * per_group + second_pick], axis=1)
        shuffle = jax.random.permutation(keys[2], DEV_ROWS)
        return pairs[shuffle]
    return jax.vmap(one_block)(jax.random.split(base, block_count)).reshape(TOKENS, 2).astype(jnp.int32)


def level_of(rng, extent, shards, least, high):
    factor_of, own = 1.0, jax.random.fold_in(rng, 6)
    for dim, blocks in shards:
        heights = jnp.exp(jax.random.uniform(jax.random.fold_in(own, dim), (blocks,), jnp.float32, least / len(shards), high / len(shards)))
        factor_of = factor_of * jnp.repeat(heights, extent[dim] // blocks).reshape([-1 if axis == dim else 1 for axis in range(len(extent))])
    return factor_of


def normal_values(rng, shape, scale, limit, shards=(), kind=jnp.bfloat16):
    level = level_of(rng, shape, shards, -0.22, 0.18) if shards else 1.0
    entries = jax.random.normal(rng, shape, jnp.float32) * scale * level
    return jnp.minimum(jnp.maximum(entries, -limit), limit).astype(kind)


def setup_inputs(seed: int = 0) -> dict:
    splits = jax.random.split(jax.random.key(seed), 16)
    return {
        "ssm_input": normal_values(splits[0], (TOKENS, SSMW), 1.0, 6.0, ((0, 16), (1, 2))),
        "lam_real": draw_lam_real(jax.random.fold_in(splits[15], 71), 0),
        "lam_imag": draw_lam_imag(jax.random.fold_in(splits[15], 71), 0),
        "state_in": draw_state_in(jax.random.fold_in(splits[15], 71), 0),
        "read_out": normal_values(splits[4], (SSMG, 2 * STATE, GROUP_CH), (2 * STATE) ** -0.5, 0.5, ((0, 2),), jnp.float32),
        "channel_skip": normal_values(splits[5], (SSMW,), 0.5, 3.0, ((0, 2),), jnp.float32),
        "glu_weight": normal_values(splits[6], (SSMW, SSMW), SSMW ** -0.5, 0.1875),
        "out_weight": normal_values(splits[7], (SSMW, D), (SSMW // 4) ** -0.5, 0.375),
        "residual": normal_values(splits[8], (TOKENS, D), 1.0, 6.0, ((0, 32),)),
        "norm_gain": jnp.clip(1.0 + 0.18 * jax.random.normal(splits[9], (D,), jnp.float32), 0.1, 1.9),
        "expert_ids": draw_expert_ids(jax.random.fold_in(splits[15], 71), 0),
        "route_weight": jnp.clip(0.25 + 0.75 * jax.random.uniform(splits[11], (TOKENS, 2), jnp.float32) ** level_of(splits[11], (TOKENS, 2), ((0, 32),), -0.2, 0.2), 0.25, 1.0),
        "expert_gate": normal_values(splits[12], (EXPERTS, D, FF), D ** -0.5, 0.125, ((0, 32),)),
        "expert_up": normal_values(splits[13], (EXPERTS, D, FF), D ** -0.5, 0.125, ((0, 32),)),
        "expert_down": normal_values(splits[14], (EXPERTS, FF, D), FF ** -0.5, 0.25, ((0, 32),)),
    }


EPSILON = 1e-06

def discretize(lam_real, lam_imag, state_in):
    magnitude = jnp.exp(lam_real)
    decay_re = magnitude * jnp.cos(lam_imag)
    decay_im = magnitude * jnp.sin(lam_imag)
    numer_re = decay_re - 1.0
    denom = lam_real * lam_real + lam_imag * lam_imag
    hold_re = ((numer_re * lam_real + decay_im * lam_imag) / denom)[:, None, :]
    hold_im = ((decay_im * lam_real - numer_re * lam_imag) / denom)[:, None, :]
    drive_re = hold_re * state_in[0] - hold_im * state_in[1]
    drive_im = hold_re * state_in[1] + hold_im * state_in[0]
    drive = jnp.concatenate([drive_re, drive_im], axis=-1).astype(jnp.bfloat16)
    return (decay_re, decay_im, drive)

def powers(lam_real, lam_imag, exponent):
    magnitude = jnp.exp(exponent[:, None, None] * lam_real[None])
    angle = exponent[:, None, None] * lam_imag[None]
    return (magnitude * jnp.cos(angle), magnitude * jnp.sin(angle))

def combine_steps(earlier, later):
    return (later[0] * earlier[0] - later[1] * earlier[1], later[0] * earlier[1] + later[1] * earlier[0], later[0] * earlier[2] - later[1] * earlier[3] + later[2], later[0] * earlier[3] + later[1] * earlier[2] + later[3])

def block_states(push_re, push_im, decay_re, decay_im):
    shape_in = push_re.shape
    flat_re = push_re.reshape(shape_in[0], -1)
    flat_im = push_im.reshape(shape_in[0], -1)
    scale_re = jnp.broadcast_to(decay_re.reshape(1, -1), flat_re.shape)
    scale_im = jnp.broadcast_to(decay_im.reshape(1, -1), flat_im.shape)
    result = lax.associative_scan(combine_steps, (scale_re, scale_im, flat_re, flat_im), axis=0)
    return (result[2].reshape(shape_in), result[3].reshape(shape_in))

def readout(part_re, part_im, read_out):
    stacked = jnp.concatenate([part_re, part_im], axis=-1)
    return jnp.einsum('tgq,gqm->tgm', stacked, read_out, precision=lax.Precision.HIGHEST)

def reference(ssm_input, lam_real, lam_imag, state_in, read_out, channel_skip, glu_weight, out_weight, residual, norm_gain, expert_ids, route_weight, expert_gate, expert_up, expert_down):
    decay_re, decay_im, drive = discretize(lam_real, lam_imag, state_in)
    block_count = TOKENS // ROWS_SP
    inputs = ssm_input.reshape(block_count, ROWS_SP, SSMG, GROUP_CH)
    skips = channel_skip.reshape(SSMG, GROUP_CH)
    ahead_re, ahead_im = powers(lam_real, lam_imag, jnp.arange(1, ROWS_SP + 1).astype(jnp.float32))

    def one_block(carry, block_input):
        carry_re, carry_im = carry
        pushed = jnp.einsum('tgm,gmp->tgp', block_input.astype(jnp.float32), drive.astype(jnp.float32), precision=lax.Precision.HIGHEST)
        state_re, state_im = block_states(pushed[..., :STATE], pushed[..., STATE:], decay_re, decay_im)
        state_re = state_re + ahead_re * carry_re - ahead_im * carry_im
        state_im = state_im + ahead_re * carry_im + ahead_im * carry_re
        read = readout(state_re, state_im, read_out)
        pre = jax.nn.gelu(read + skips * block_input.astype(jnp.float32)).astype(jnp.bfloat16)
        return ((state_re[-1], state_im[-1]), pre)
    start = (jnp.zeros((SSMG, STATE), jnp.float32), jnp.zeros((SSMG, STATE), jnp.float32))
    _, pre = lax.scan(one_block, start, inputs)
    pre = pre.reshape(TOKENS, SSMW)
    gate_lin = jnp.dot(pre, glu_weight, preferred_element_type=jnp.float32)
    gated = (pre.astype(jnp.float32) * jax.nn.sigmoid(gate_lin)).astype(jnp.bfloat16)
    mixed = residual.astype(jnp.float32) + jnp.dot(gated, out_weight, preferred_element_type=jnp.float32)
    normed = (mixed * lax.rsqrt(lax.optimization_barrier(jnp.mean(mixed * mixed, axis=-1, keepdims=True)) + EPSILON) * norm_gain).astype(jnp.bfloat16)
    device_count = N_SP * N_TP
    route_count = expert_ids.shape[1]
    slot_ids = expert_ids.reshape(device_count, DEV_ROWS * route_count)
    onehot = (slot_ids[:, :, None] == jnp.arange(EXPERTS, dtype=jnp.int32)[None, None, :]).astype(jnp.int32)
    rank = lax.optimization_barrier(jnp.sum(jnp.cumsum(onehot, axis=1) * onehot, axis=2)) - 1
    position = ((slot_ids * device_count + jnp.arange(device_count, dtype=jnp.int32)[:, None]) * CAP + rank).reshape(-1).astype(jnp.int32)
    slot_total = EXPERTS * device_count * CAP
    token_of = jnp.zeros((slot_total,), jnp.int32).at[position].set((jnp.arange(TOKENS * route_count) // route_count).astype(jnp.int32))
    weight_of = jnp.zeros((slot_total,), jnp.float32).at[position].set(route_weight.reshape(-1))
    per_expert = device_count * CAP

    def one_expert(expert, accum):
        start_at = (expert * per_expert).astype(jnp.int32)
        chosen = lax.dynamic_slice_in_dim(token_of, start_at, per_expert)
        weights = lax.dynamic_slice_in_dim(weight_of, start_at, per_expert)
        rows_in = normed[chosen]
        gate_part = jnp.dot(rows_in, expert_gate[expert], preferred_element_type=jnp.float32)
        up_part = jnp.dot(rows_in, expert_up[expert], preferred_element_type=jnp.float32)
        hidden = (jax.nn.silu(gate_part) * up_part).astype(jnp.bfloat16)
        answer = jnp.dot(hidden, expert_down[expert], preferred_element_type=jnp.float32).astype(jnp.bfloat16)
        return accum.at[chosen].add(answer.astype(jnp.float32) * weights[:, None])
    accum = lax.fori_loop(0, EXPERTS, one_expert, jnp.zeros((TOKENS, D), jnp.float32))
    return (mixed + accum).astype(jnp.bfloat16)
```

```python
import functools

import jax
import jax.numpy as jnp
from jax import lax
from jax.experimental import pallas as pl
from jax.experimental.pallas import tpu as pltpu
from jax.sharding import PartitionSpec as P

GROUPS = 4
EPSILON = 1e-06
LANES = 128
SEGMENTS = 8


def discretize(lam_real, lam_imag, state_in):
    magnitude = jnp.exp(lam_real)
    decay_re = magnitude * jnp.cos(lam_imag)
    decay_im = magnitude * jnp.sin(lam_imag)
    numer_re = decay_re - 1.0
    denom = lam_real * lam_real + lam_imag * lam_imag
    hold_re = ((numer_re * lam_real + decay_im * lam_imag) / denom)[:, None, :]
    hold_im = ((decay_im * lam_real - numer_re * lam_imag) / denom)[:, None, :]
    drive_re = hold_re * state_in[0] - hold_im * state_in[1]
    drive_im = hold_re * state_in[1] + hold_im * state_in[0]
    return drive_re.astype(jnp.bfloat16), drive_im.astype(jnp.bfloat16)


def powers(lam_real, lam_imag, exponent):
    magnitude = jnp.exp(exponent[:, None, None] * lam_real[None])
    angle = exponent[:, None, None] * lam_imag[None]
    return (magnitude * jnp.cos(angle), magnitude * jnp.sin(angle))


def iota(shape, dim):
    return lax.broadcasted_iota(jnp.int32, shape, dim)


def times(a_re, a_im, b_re, b_im):
    return a_re * b_re - a_im * b_im, a_re * b_im + a_im * b_re


def segment_order(rows, back=False):
    length = rows // SEGMENTS
    ordered, token = iota((rows, rows), 1 if back else 0), iota((rows, rows), 0 if back else 1)
    same = (ordered % SEGMENTS) * length + ordered // SEGMENTS == token
    return same.astype(jnp.float32).astype(jnp.bfloat16)


def spread(block, copies, row_group, column_group):
    rows, width = block.shape
    wide = width * copies
    pick = iota((width, wide), 0) == iota((width, wide), 1) % width
    tiled = jnp.dot(
        block, pick.astype(jnp.float32).astype(jnp.bfloat16), preferred_element_type=jnp.float32
    )
    keep = (iota((rows, wide), 0) // row_group) == (iota((rows, wide), 1) // column_group)
    return jnp.where(keep, tiled, 0.0).astype(jnp.bfloat16)


def ssm_ordered(x_ref):
    rows = x_ref.shape[0]
    return jnp.dot(
        segment_order(rows), x_ref[...], preferred_element_type=jnp.float32
    )


def fill_push(x_tile, drive_re_ref, drive_im_ref, tile, channels, push):
    states = drive_re_ref.shape[1]
    copies = LANES // channels
    width = copies * states
    rows = pl.ds(tile * LANES, LANES)
    for part, ref in enumerate((drive_re_ref, drive_im_ref)):
        block = spread(ref[rows, :], copies, channels, states)
        push[:, part * width : (part + 1) * width] = jnp.dot(
            x_tile, block, preferred_element_type=jnp.float32
        )


def run_scan(push, width, decay_re, decay_im, start_re, start_im, keep):
    shape = (SEGMENTS, width)
    decay_re = jnp.broadcast_to(decay_re, shape)
    decay_im = jnp.broadcast_to(decay_im, shape)

    def step(j, carry):
        rows = pl.ds(pl.multiple_of(j * SEGMENTS, SEGMENTS), SEGMENTS)
        next_re, next_im = times(decay_re, decay_im, *carry)
        next_re = next_re + push[rows, :width]
        next_im = next_im + push[rows, width:]
        if keep:
            push[rows, :width] = next_re
            push[rows, width:] = next_im
        return next_re, next_im

    return lax.fori_loop(0, push.shape[0] // SEGMENTS, step, (start_re, start_im), unroll=4)


def ends_kernel(channels, x_ref, drive_re_ref, drive_im_ref, pow_re_ref, pow_im_ref,
                ends_re_ref, ends_im_ref, final_ref, push):
    ordered = ssm_ordered(x_ref).astype(jnp.bfloat16)
    width = push.shape[1] // 2
    total = pow_re_ref.shape[1]
    for tile in range(total // width):
        lanes = slice(tile * width, (tile + 1) * width)
        fill_push(
            ordered[:, tile * LANES : (tile + 1) * LANES], drive_re_ref, drive_im_ref, tile,
            channels, push,
        )
        zero = jnp.zeros((SEGMENTS, width), jnp.float32)
        end_re, end_im = run_scan(
            push, width, pow_re_ref[0:1, lanes], pow_im_ref[0:1, lanes], zero, zero, False
        )
        ends_re_ref[:, lanes] = end_re
        ends_im_ref[:, lanes] = end_im
        seg_re, seg_im = pow_re_ref[1:2, lanes], pow_im_ref[1:2, lanes]
        sum_re, sum_im = end_re[0:1], end_im[0:1]
        for s in range(1, SEGMENTS):
            sum_re, sum_im = times(seg_re, seg_im, sum_re, sum_im)
            sum_re, sum_im = sum_re + end_re[s : s + 1], sum_im + end_im[s : s + 1]
        final_ref[0:1, lanes] = sum_re
        final_ref[1:2, lanes] = sum_im


def mixer_kernel(channels, x_ref, drive_re_ref, drive_im_ref, pow_re_ref, pow_im_ref,
                 ends_re_ref, ends_im_ref, finals_ref, read_ref, skip_ref, out_ref,
                 push, start, pre):
    mine = lax.axis_index("sp")
    wide = ssm_ordered(x_ref)
    ordered = wide.astype(jnp.bfloat16)
    rows = x_ref.shape[0]
    width = push.shape[1] // 2
    total = pow_re_ref.shape[1]
    states = drive_re_ref.shape[1]
    copies = LANES // channels
    for tile in range(total // width):
        lanes = slice(tile * width, (tile + 1) * width)
        span_re, span_im = pow_re_ref[2:3, lanes], pow_im_ref[2:3, lanes]
        zero = jnp.zeros((1, width), jnp.float32)

        def hop(position, so_far):
            new_re, new_im = times(span_re, span_im, *so_far)
            return (new_re + finals_ref[position, 0:1, lanes],
                    new_im + finals_ref[position, 1:2, lanes])

        in_re, in_im = lax.fori_loop(0, mine, hop, (zero, zero))
        seg_re, seg_im = pow_re_ref[1:2, lanes], pow_im_ref[1:2, lanes]
        for s in range(SEGMENTS):
            start[s : s + 1, :width] = in_re
            start[s : s + 1, width:] = in_im
            in_re, in_im = times(seg_re, seg_im, in_re, in_im)
            in_re = in_re + ends_re_ref[s : s + 1, lanes]
            in_im = in_im + ends_im_ref[s : s + 1, lanes]
        own = slice(tile * LANES, (tile + 1) * LANES)
        fill_push(ordered[:, own], drive_re_ref, drive_im_ref, tile, channels, push)
        run_scan(
            push, width, pow_re_ref[0:1, lanes], pow_im_ref[0:1, lanes], start[:, :width],
            start[:, width:], True,
        )
        read = jnp.zeros((rows, LANES), jnp.float32)
        for part in range(2):
            block = read_ref[tile * copies : (tile + 1) * copies,
                             part * states : (part + 1) * states, :]
            block = block.reshape(width, channels).astype(jnp.bfloat16)
            block = spread(block, copies, states, channels)
            read = read + jnp.dot(
                push[:, part * width : (part + 1) * width].astype(jnp.bfloat16), block,
                preferred_element_type=jnp.float32,
            )
        value = jax.nn.gelu(read + skip_ref[0:1, own] * wide[:, own])
        pre[:, own] = value.astype(jnp.bfloat16)
    out_ref[...] = jnp.dot(
        segment_order(rows, back=True), pre[...], preferred_element_type=jnp.float32
    ).astype(jnp.bfloat16)


def mixer(ssm_input, lam_real, lam_imag, state_in, read_out, channel_skip):
    rows, width_in = ssm_input.shape
    groups, states = lam_real.shape
    channels = state_in.shape[2]
    total = groups * states
    width = (LANES // channels) * states
    drive_re, drive_im = discretize(lam_real, lam_imag, state_in)
    drive_re = drive_re.reshape(width_in, states)
    drive_im = drive_im.reshape(width_in, states)
    steps = jnp.asarray([1.0, rows // SEGMENTS, rows], jnp.float32)
    pow_re, pow_im = powers(lam_real, lam_imag, steps)
    pow_re, pow_im = pow_re.reshape(3, total), pow_im.reshape(3, total)
    f32 = jnp.float32
    ends_re, ends_im, final = pl.pallas_call(
        functools.partial(ends_kernel, channels),
        out_shape=(
            jax.ShapeDtypeStruct((SEGMENTS, total), f32),
            jax.ShapeDtypeStruct((SEGMENTS, total), f32),
            jax.ShapeDtypeStruct((2, total), f32),
        ),
        scratch_shapes=[pltpu.VMEM((rows, 2 * width), f32)],
        name="ends",
    )(ssm_input, drive_re, drive_im, pow_re, pow_im)
    finals = lax.all_gather(final, "sp")
    return pl.pallas_call(
        functools.partial(mixer_kernel, channels),
        out_shape=jax.ShapeDtypeStruct((rows, width_in), jnp.bfloat16),
        scratch_shapes=[
            pltpu.VMEM((rows, 2 * width), f32),
            pltpu.VMEM((SEGMENTS, 2 * width), f32),
            pltpu.VMEM((rows, width_in), jnp.bfloat16),
        ],
        name="mixer",
    )(ssm_input, drive_re, drive_im, pow_re, pow_im, ends_re, ends_im, finals, read_out,
      channel_skip.reshape(1, width_in))


def swap_halves(pre):
    half = pre.shape[0] // 2
    me = lax.axis_index("tp")
    kept = lax.dynamic_slice_in_dim(pre, me * half, half, 0)
    given = lax.dynamic_slice_in_dim(pre, (1 - me) * half, half, 0)
    taken = lax.ppermute(given, "tp", [(0, 1), (1, 0)])
    first = jnp.where(me == 0, kept, taken)
    second = jnp.where(me == 0, taken, kept)
    return jnp.concatenate([first, second], axis=1)


def routes(expert_ids, expert_count, capacity):
    tokens = expert_ids.shape[0]
    experts = jnp.arange(expert_count, dtype=jnp.int32)
    onehot = (expert_ids[:, :, None] == experts[None, None, :]).astype(jnp.float32)
    earlier = (jnp.arange(tokens)[:, None] > jnp.arange(tokens)[None, :]).astype(jnp.bfloat16)
    before = jnp.dot(
        earlier, jnp.sum(onehot, axis=1).astype(jnp.bfloat16), preferred_element_type=jnp.float32
    )
    rank = jnp.sum(before[:, None, :] * onehot, axis=-1).astype(jnp.int32)
    return expert_ids * capacity + rank


def run_expert(rows, expert_gate, expert_up, expert_down):
    gate_part = jnp.dot(rows, expert_gate[0], preferred_element_type=jnp.float32)
    up_part = jnp.dot(rows, expert_up[0], preferred_element_type=jnp.float32)
    hidden = (jax.nn.silu(gate_part) * up_part).astype(jnp.bfloat16)
    return jnp.dot(hidden, expert_down[0], preferred_element_type=jnp.float32).astype(
        jnp.bfloat16
    )


def on_device(
    ssm_input,
    lam_real,
    lam_imag,
    state_in,
    read_out,
    channel_skip,
    glu_weight,
    out_weight,
    residual,
    norm_gain,
    expert_ids,
    route_weight,
    expert_gate,
    expert_up,
    expert_down,
):
    f32, bf16 = jnp.float32, jnp.bfloat16
    pre = mixer(ssm_input, lam_real, lam_imag, state_in, read_out, channel_skip)
    own_tokens = swap_halves(pre)
    gate_lin = jnp.dot(own_tokens, glu_weight, preferred_element_type=f32)
    gated = (own_tokens.astype(f32) * jax.nn.sigmoid(gate_lin)).astype(bf16)
    mixed = residual.astype(f32) + jnp.dot(gated, out_weight, preferred_element_type=f32)
    normed = (
        mixed * lax.rsqrt(jnp.mean(mixed * mixed, axis=-1, keepdims=True) + EPSILON) * norm_gain
    ).astype(bf16)
    tokens, model_width = normed.shape
    expert_count = lax.axis_size("sp") * lax.axis_size("tp")
    capacity = tokens * GROUPS // expert_count
    position = routes(expert_ids, expert_count, capacity)
    slots = jnp.arange(expert_count * capacity, dtype=jnp.int32)
    chosen = position[:, :, None] == slots[None, None, :]
    pick = jnp.any(chosen, axis=1).astype(bf16)
    outgoing = lax.dot_general(
        pick, normed, (((0,), (0,)), ((), ())), preferred_element_type=f32
    ).astype(bf16)
    outgoing = outgoing.reshape(expert_count, capacity, model_width)
    arrived = lax.all_to_all(outgoing, ("sp", "tp"), split_axis=0, concat_axis=0, tiled=True)
    answered = run_expert(
        arrived.reshape(-1, model_width), expert_gate, expert_up, expert_down
    ).reshape(arrived.shape)
    returned = lax.all_to_all(answered, ("sp", "tp"), split_axis=0, concat_axis=0, tiled=True)
    returned = returned.reshape(-1, model_width)
    weights = jnp.sum(jnp.where(chosen, route_weight[:, :, None], 0.0), axis=1)
    coarse = weights.astype(bf16)
    fine = (weights - coarse.astype(f32)).astype(bf16)
    routed = jnp.dot(coarse, returned, preferred_element_type=f32) + jnp.dot(
        fine, returned, preferred_element_type=f32
    )
    return (mixed + routed).astype(bf16)


def solution(mesh):
    placed = (
        P("sp", "tp"),
        P("tp", None),
        P("tp", None),
        P(None, "tp", None, None),
        P("tp", None, None),
        P("tp"),
        P(),
        P(),
        P(("sp", "tp"), None),
        P(),
        P(("sp", "tp"), None),
        P(("sp", "tp"), None),
        P(("sp", "tp"), None, None),
        P(("sp", "tp"), None, None),
        P(("sp", "tp"), None, None),
    )
    return jax.shard_map(
        on_device, mesh=mesh, in_specs=placed, out_specs=P(("sp", "tp"), None), check_vma=False
    )
```

```python
import functools

import jax
import jax.numpy as jnp
from jax import lax
from jax.experimental import pallas as pl
from jax.experimental.pallas import tpu as pltpu
from jax.sharding import PartitionSpec as P

GROUPS = 4
EPSILON = 1e-06
LANES = 128
SEGMENTS = 8


def discretize(lam_real, lam_imag, state_in):
    magnitude = jnp.exp(lam_real)
    decay_re = magnitude * jnp.cos(lam_imag)
    decay_im = magnitude * jnp.sin(lam_imag)
    numer_re = decay_re - 1.0
    denom = lam_real * lam_real + lam_imag * lam_imag
    hold_re = ((numer_re * lam_real + decay_im * lam_imag) / denom)[:, None, :]
    hold_im = ((decay_im * lam_real - numer_re * lam_imag) / denom)[:, None, :]
    drive_re = hold_re * state_in[0] - hold_im * state_in[1]
    drive_im = hold_re * state_in[1] + hold_im * state_in[0]
    return drive_re.astype(jnp.bfloat16), drive_im.astype(jnp.bfloat16)


def powers(lam_real, lam_imag, exponent):
    magnitude = jnp.exp(exponent[:, None, None] * lam_real[None])
    angle = exponent[:, None, None] * lam_imag[None]
    return (magnitude * jnp.cos(angle), magnitude * jnp.sin(angle))


def iota(shape, dim):
    return lax.broadcasted_iota(jnp.int32, shape, dim)


def times(a_re, a_im, b_re, b_im):
    return a_re * b_re - a_im * b_im, a_re * b_im + a_im * b_re


def segment_order(rows, back=False):
    length = rows // SEGMENTS
    ordered, token = iota((rows, rows), 1 if back else 0), iota((rows, rows), 0 if back else 1)
    same = (ordered % SEGMENTS) * length + ordered // SEGMENTS == token
    return same.astype(jnp.float32).astype(jnp.bfloat16)


def spread(block, copies, row_group, column_group):
    rows, width = block.shape
    wide = width * copies
    pick = iota((width, wide), 0) == iota((width, wide), 1) % width
    tiled = jnp.dot(
        block, pick.astype(jnp.float32).astype(jnp.bfloat16), preferred_element_type=jnp.float32
    )
    keep = (iota((rows, wide), 0) // row_group) == (iota((rows, wide), 1) // column_group)
    return jnp.where(keep, tiled, 0.0).astype(jnp.bfloat16)


def ssm_ordered(x_ref):
    rows = x_ref.shape[0]
    return jnp.dot(
        segment_order(rows), x_ref[...], preferred_element_type=jnp.float32
    )


def fill_push(x_tile, drive_re_ref, drive_im_ref, tile, channels, push):
    states = drive_re_ref.shape[1]
    copies = LANES // channels
    width = copies * states
    rows = pl.ds(tile * LANES, LANES)
    for part, ref in enumerate((drive_re_ref, drive_im_ref)):
        block = spread(ref[rows, :], copies, channels, states)
        push[:, part * width : (part + 1) * width] = jnp.dot(
            x_tile, block, preferred_element_type=jnp.float32
        )


def run_scan(push, width, decay_re, decay_im, start_re, start_im, keep):
    shape = (SEGMENTS, width)
    decay_re = jnp.broadcast_to(decay_re, shape)
    decay_im = jnp.broadcast_to(decay_im, shape)

    def step(j, carry):
        rows = pl.ds(pl.multiple_of(j * SEGMENTS, SEGMENTS), SEGMENTS)
        next_re, next_im = times(decay_re, decay_im, *carry)
        next_re = next_re + push[rows, :width]
        next_im = next_im + push[rows, width:]
        if keep:
            push[rows, :width] = next_re
            push[rows, width:] = next_im
        return next_re, next_im

    return lax.fori_loop(0, push.shape[0] // SEGMENTS, step, (start_re, start_im), unroll=4)


MESH = pl.DeviceIdType.MESH


def mixer_kernel(channels, sp_count, x_ref, drive_re_ref, drive_im_ref, pow_re_ref, pow_im_ref,
                 read_ref, skip_ref, out_ref, push, start, pre, ends_re, ends_im, final, finals,
                 halves, taken, send_sem, recv_sem, swap_sem):
    mine, core = lax.axis_index("sp"), lax.axis_index("tp")

    def peer(step):
        return (lax.rem(mine + step, sp_count), core)

    barrier = pltpu.get_barrier_semaphore()

    @pl.loop(1, sp_count)
    def _(step):
        pl.semaphore_signal(barrier, inc=1, device_id=peer(step), device_id_type=MESH)

    pl.semaphore_signal(barrier, inc=1, device_id=(mine, 1 - core), device_id_type=MESH)

    wide = ssm_ordered(x_ref)
    ordered = wide.astype(jnp.bfloat16)
    rows = x_ref.shape[0]
    width = push.shape[2] // 2
    total = pow_re_ref.shape[1]
    states = drive_re_ref.shape[1]
    copies = LANES // channels
    for tile in range(total // width):
        lanes = slice(tile * width, (tile + 1) * width)
        fill_push(
            ordered[:, tile * LANES : (tile + 1) * LANES], drive_re_ref, drive_im_ref, tile,
            channels, push.at[tile],
        )
        zero = jnp.zeros((SEGMENTS, width), jnp.float32)
        end_re, end_im = run_scan(
            push.at[tile], width, pow_re_ref[0:1, lanes], pow_im_ref[0:1, lanes], zero, zero,
            False,
        )
        ends_re[:, lanes] = end_re
        ends_im[:, lanes] = end_im
        seg_re, seg_im = pow_re_ref[1:2, lanes], pow_im_ref[1:2, lanes]
        sum_re, sum_im = end_re[0:1], end_im[0:1]
        for s in range(1, SEGMENTS):
            sum_re, sum_im = times(seg_re, seg_im, sum_re, sum_im)
            sum_re, sum_im = sum_re + end_re[s : s + 1], sum_im + end_im[s : s + 1]
        final[0:1, lanes] = sum_re
        final[1:2, lanes] = sum_im

    pl.semaphore_wait(barrier, sp_count)

    def give(step):
        return pltpu.make_async_remote_copy(
            src_ref=final, dst_ref=finals.at[mine], send_sem=send_sem.at[step],
            recv_sem=recv_sem.at[step], device_id=peer(step), device_id_type=MESH,
        )

    @pl.loop(1, sp_count)
    def _(step):
        give(step).start()

    @pl.loop(1, sp_count)
    def _(step):
        give(step).wait()

    for tile in range(total // width):
        lanes = slice(tile * width, (tile + 1) * width)
        span_re, span_im = pow_re_ref[2:3, lanes], pow_im_ref[2:3, lanes]
        zero = jnp.zeros((1, width), jnp.float32)

        def hop(position, so_far):
            new_re, new_im = times(span_re, span_im, *so_far)
            return (new_re + finals[position, 0:1, lanes], new_im + finals[position, 1:2, lanes])

        in_re, in_im = lax.fori_loop(0, mine, hop, (zero, zero))
        seg_re, seg_im = pow_re_ref[1:2, lanes], pow_im_ref[1:2, lanes]
        for s in range(SEGMENTS):
            start[s : s + 1, :width] = in_re
            start[s : s + 1, width:] = in_im
            in_re, in_im = times(seg_re, seg_im, in_re, in_im)
            in_re = in_re + ends_re[s : s + 1, lanes]
            in_im = in_im + ends_im[s : s + 1, lanes]
        own = slice(tile * LANES, (tile + 1) * LANES)
        run_scan(
            push.at[tile], width, pow_re_ref[0:1, lanes], pow_im_ref[0:1, lanes],
            start[:, :width], start[:, width:], True,
        )
        read = jnp.zeros((rows, LANES), jnp.float32)
        for part in range(2):
            block = read_ref[tile * copies : (tile + 1) * copies,
                             part * states : (part + 1) * states, :]
            block = block.reshape(width, channels).astype(jnp.bfloat16)
            block = spread(block, copies, states, channels)
            read = read + jnp.dot(
                push[tile, :, part * width : (part + 1) * width].astype(jnp.bfloat16), block,
                preferred_element_type=jnp.float32,
            )
        value = jax.nn.gelu(read + skip_ref[0:1, own] * wide[:, own])
        pre[:, own] = value.astype(jnp.bfloat16)
    half = rows // 2
    back = jnp.dot(
        segment_order(rows, back=True), pre[...], preferred_element_type=jnp.float32
    ).astype(jnp.bfloat16)
    halves[0] = back[:half]
    halves[1] = back[half:]
    swap = pltpu.make_async_remote_copy(
        src_ref=halves.at[1 - core], dst_ref=taken, send_sem=swap_sem.at[0],
        recv_sem=swap_sem.at[1], device_id=(mine, 1 - core), device_id_type=MESH,
    )
    swap.start()
    wide_in = x_ref.shape[1]
    out_ref[:, pl.ds(pl.multiple_of(core * wide_in, LANES), wide_in)] = halves[core]
    swap.wait()
    out_ref[:, pl.ds(pl.multiple_of((1 - core) * wide_in, LANES), wide_in)] = taken[...]


def mixer(ssm_input, lam_real, lam_imag, state_in, read_out, channel_skip):
    rows, width_in = ssm_input.shape
    groups, states = lam_real.shape
    channels = state_in.shape[2]
    sp_count = lax.axis_size("sp")
    total = groups * states
    width = (LANES // channels) * states
    drive_re, drive_im = discretize(lam_real, lam_imag, state_in)
    drive_re = drive_re.reshape(width_in, states)
    drive_im = drive_im.reshape(width_in, states)
    steps = jnp.asarray([1.0, rows // SEGMENTS, rows], jnp.float32)
    pow_re, pow_im = powers(lam_real, lam_imag, steps)
    pow_re, pow_im = pow_re.reshape(3, total), pow_im.reshape(3, total)
    f32, bf16 = jnp.float32, jnp.bfloat16
    return pl.pallas_call(
        functools.partial(mixer_kernel, channels, sp_count),
        out_shape=jax.ShapeDtypeStruct((rows // 2, width_in * 2), bf16),
        scratch_shapes=[
            pltpu.VMEM((total // width, rows, 2 * width), f32),
            pltpu.VMEM((SEGMENTS, 2 * width), f32),
            pltpu.VMEM((rows, width_in), bf16),
            pltpu.VMEM((SEGMENTS, total), f32),
            pltpu.VMEM((SEGMENTS, total), f32),
            pltpu.VMEM((2, total), f32),
            pltpu.VMEM((sp_count, 2, total), f32),
            pltpu.VMEM((2, rows // 2, width_in), bf16),
            pltpu.VMEM((rows // 2, width_in), bf16),
            pltpu.SemaphoreType.DMA((sp_count,)),
            pltpu.SemaphoreType.DMA((sp_count,)),
            pltpu.SemaphoreType.DMA((2,)),
        ],
        compiler_params=pltpu.CompilerParams(collective_id=0, has_side_effects=True),
        name="mixer",
    )(ssm_input, drive_re, drive_im, pow_re, pow_im, read_out, channel_skip.reshape(1, width_in))


def place(meta, slots, weigh):
    tokens = meta.shape[1]
    slot = iota((slots, tokens), 0).astype(jnp.float32)
    total = jnp.zeros((slots, tokens), jnp.float32)
    for k in range(2):
        value = meta[2 + k : 3 + k] if weigh else 1.0
        total = total + jnp.where(slot == meta[k : k + 1], value, 0.0)
    return total


def experts_kernel(planes, members, cores, rows_ref, meta_ref, mixed_ref, gather_ref,
                   gate_hbm, up_hbm, down_hbm, out_ref, gate, up, down, got, got_meta, sent,
                   arrived, answer, back, joined, home, load_sem, z_send, z_recv, m_send, m_recv,
                   out_send, out_recv, ret_send, ret_recv, home_send, home_recv):
    f32, bf16 = jnp.float32, jnp.bfloat16
    loads = [
        pltpu.make_async_copy(hbm.at[0], vmem, load_sem.at[i])
        for i, (hbm, vmem) in enumerate(((gate_hbm, gate), (up_hbm, up), (down_hbm, down)))
    ]
    for load in loads:
        load.start()
    sp, core = lax.axis_index("sp"), lax.axis_index("tp")
    per_plane = members // cores
    plane = sp // per_plane
    column = sp - plane * per_plane
    member = column * cores + core

    def plane_at(step):
        return lax.rem(plane + step, planes)

    def above(step):
        return (plane_at(step) * per_plane + column, core)

    def member_at(step):
        return lax.rem(member + step, members)

    def beside(step):
        other = member_at(step)
        return (plane * per_plane + other // cores, lax.rem(other, cores))

    barrier = pltpu.get_barrier_semaphore()

    @pl.loop(1, planes)
    def _(step):
        pl.semaphore_signal(barrier, inc=1, device_id=above(step), device_id_type=MESH)

    @pl.loop(1, members)
    def _(step):
        pl.semaphore_signal(barrier, inc=1, device_id=beside(step), device_id_type=MESH)

    pl.semaphore_wait(barrier, planes + members - 2)

    def remote(src, dst, send, recv, where):
        return pltpu.make_async_remote_copy(
            src_ref=src, dst_ref=dst, send_sem=send, recv_sem=recv, device_id=where,
            device_id_type=MESH,
        )

    def meta_copy(d):
        return remote(meta_ref.at[plane_at(d)], got_meta.at[d], m_send.at[d], m_recv.at[d],
                      above(d))

    def rows_copy(d):
        return remote(rows_ref.at[plane_at(d)], got.at[d], z_send.at[d], z_recv.at[d], above(d))

    def out_copy(d, step):
        return remote(sent.at[d, member_at(step)], arrived.at[d, member], out_send.at[d, step],
                      out_recv.at[d, step], beside(step))

    def ret_copy(d, step):
        return remote(answer.at[d, member_at(step)], back.at[d, member], ret_send.at[d, step],
                      ret_recv.at[d, step], beside(step))

    def home_copy(d):
        return remote(joined.at[d], home.at[d], home_send.at[d], home_recv.at[d],
                      above(planes - d))

    for d in range(1, planes):
        meta_copy(d).start()
    for d in range(1, planes):
        rows_copy(d).start()

    capacity, model_width = sent.shape[2], sent.shape[3]
    slots = members * capacity
    tokens = rows_ref.shape[1]

    def dispatch(d):
        if d:
            meta_copy(d).wait_recv()
            rows_copy(d).wait_recv()
            block, meta = got[d], got_meta[d]
        else:
            block, meta = rows_ref[plane], meta_ref[plane]
        pick = place(meta[:, :tokens], slots, False).astype(bf16)
        spread_rows = jnp.dot(pick, block, preferred_element_type=f32).astype(bf16)
        sent[d] = spread_rows.reshape(members, capacity, model_width)

        @pl.loop(1, members)
        def _(step):
            out_copy(d, step).start()

        arrived[d, member] = sent[d, member]

    def expert(d):
        if d == 0:
            for load in loads:
                load.wait()

        @pl.loop(1, members)
        def _(step):
            out_copy(d, step).wait_recv()

        rows = arrived[d].reshape(slots, model_width)
        gate_part = jnp.dot(rows, gate[...], preferred_element_type=f32)
        up_part = jnp.dot(rows, up[...], preferred_element_type=f32)
        hidden = (jax.nn.silu(gate_part) * up_part).astype(bf16)
        result = jnp.dot(hidden, down[...], preferred_element_type=f32).astype(bf16)
        answer[d] = result.reshape(members, capacity, model_width)

        @pl.loop(1, members)
        def _(step):
            ret_copy(d, step).start()

        back[d, member] = answer[d, member]

    def join(d):
        @pl.loop(1, members)
        def _(step):
            ret_copy(d, step).wait_recv()

        meta = got_meta[d] if d else meta_ref[plane]
        weights = place(meta[:, :tokens], slots, True)
        coarse = weights.astype(bf16)
        fine = (weights - coarse.astype(f32)).astype(bf16)
        answers = back[d].reshape(slots, model_width)
        over_slots = (((0,), (0,)), ((), ()))
        total = lax.dot_general(coarse, answers, over_slots, preferred_element_type=f32)
        total = total + lax.dot_general(fine, answers, over_slots, preferred_element_type=f32)
        if d:
            joined[d] = total.astype(bf16)
            home_copy(d).start()
        else:
            home[0] = total.astype(bf16)

    dispatch(0)
    expert(0)
    for d in range(1, planes):
        dispatch(d)
        expert(d)
        join(d - 1)
    join(planes - 1)

    total = mixed_ref[...]
    for d in range(planes):
        if d:
            home_copy(d).wait_recv()
        total = total + jnp.dot(
            gather_ref[plane_at(d)], home[d], preferred_element_type=f32
        )
    out_ref[...] = total.astype(bf16)

    for d in range(1, planes):
        meta_copy(d).wait_send()
        rows_copy(d).wait_send()
        home_copy(d).wait_send()

    for d in range(planes):
        @pl.loop(1, members)
        def _(step):
            out_copy(d, step).wait_send()
            ret_copy(d, step).wait_send()


def earlier_count(onehot):
    tokens = onehot.shape[0]
    earlier = (jnp.arange(tokens)[:, None] > jnp.arange(tokens)[None, :]).astype(jnp.bfloat16)
    return jnp.dot(earlier, onehot.astype(jnp.bfloat16), preferred_element_type=jnp.float32)


def routes(expert_ids, route_weight, members, capacity, room, padded):
    tokens = expert_ids.shape[0]
    count = members * GROUPS
    f32 = jnp.float32
    onehot = (expert_ids[:, :, None] == jnp.arange(count, dtype=jnp.int32)).astype(f32)
    both = jnp.sum(onehot, axis=1)
    group = expert_ids[:, 0] // members
    in_group = (group[:, None] == jnp.arange(GROUPS, dtype=jnp.int32)).astype(f32)
    before = earlier_count(jnp.concatenate([both, in_group], axis=1))
    rank = jnp.sum(before[:, None, :count] * onehot, axis=-1)
    slot = (expert_ids - group[:, None] * members).astype(f32) * padded + rank
    row = group * room + jnp.sum(before[:, count:] * in_group, axis=1).astype(jnp.int32)
    mine = row[None, :] == jnp.arange(GROUPS * room, dtype=jnp.int32)[:, None]
    values = jnp.concatenate([slot + 1.0, route_weight], axis=1)
    meta = jnp.sum(jnp.where(mine[None], values.T[:, None, :], 0.0), axis=-1)
    meta = meta - jnp.asarray([1.0, 1.0, 0.0, 0.0], f32)[:, None]
    meta = meta.reshape(4, GROUPS, room).transpose(1, 0, 2)
    meta = jnp.pad(meta, ((0, 0), (0, 4), (0, -room % LANES)))
    return mine.astype(jnp.bfloat16), meta


def experts(normed, mixed, expert_ids, route_weight, expert_gate, expert_up, expert_down):
    f32, bf16 = jnp.float32, jnp.bfloat16
    tokens, model_width = normed.shape
    hidden = expert_gate.shape[2]
    cores = lax.axis_size("tp")
    members = lax.axis_size("sp") * cores // GROUPS
    capacity = tokens // members
    room = members * capacity // expert_ids.shape[1]
    padded = -(-capacity // 16) * 16
    mine, meta = routes(expert_ids, route_weight, members, capacity, room, padded)
    rows = jnp.dot(mine, normed, preferred_element_type=f32).astype(bf16)
    rows = rows.reshape(GROUPS, room, model_width)
    gather = mine.reshape(GROUPS, room, tokens).transpose(0, 2, 1)
    vmem = pl.BlockSpec(memory_space=pltpu.VMEM)
    hbm = pl.BlockSpec(memory_space=pl.ANY)
    block = pltpu.VMEM((GROUPS, members, padded, model_width), bf16)
    group_rows = pltpu.VMEM((GROUPS, room, model_width), bf16)
    dma = pltpu.SemaphoreType.DMA
    return pl.pallas_call(
        functools.partial(experts_kernel, GROUPS, members, cores),
        out_shape=jax.ShapeDtypeStruct((tokens, model_width), bf16),
        in_specs=[vmem] * 4 + [hbm] * 3,
        out_specs=vmem,
        scratch_shapes=[
            pltpu.VMEM((model_width, hidden), bf16),
            pltpu.VMEM((model_width, hidden), bf16),
            pltpu.VMEM((hidden, model_width), bf16),
            group_rows,
            pltpu.VMEM(meta.shape, f32),
            block, block, block, block,
            group_rows, group_rows,
            dma((3,)),
            dma((GROUPS,)), dma((GROUPS,)), dma((GROUPS,)), dma((GROUPS,)),
            dma((GROUPS, members)), dma((GROUPS, members)),
            dma((GROUPS, members)), dma((GROUPS, members)),
            dma((GROUPS,)), dma((GROUPS,)),
        ],
        compiler_params=pltpu.CompilerParams(collective_id=1, has_side_effects=True),
        name="experts",
    )(rows, meta, mixed, gather, expert_gate, expert_up, expert_down)


def on_device(
    ssm_input,
    lam_real,
    lam_imag,
    state_in,
    read_out,
    channel_skip,
    glu_weight,
    out_weight,
    residual,
    norm_gain,
    expert_ids,
    route_weight,
    expert_gate,
    expert_up,
    expert_down,
):
    f32, bf16 = jnp.float32, jnp.bfloat16
    own_tokens = mixer(ssm_input, lam_real, lam_imag, state_in, read_out, channel_skip)
    gate_lin = jnp.dot(own_tokens, glu_weight, preferred_element_type=f32)
    gated = (own_tokens.astype(f32) * jax.nn.sigmoid(gate_lin)).astype(bf16)
    mixed = residual.astype(f32) + jnp.dot(gated, out_weight, preferred_element_type=f32)
    normed = (
        mixed * lax.rsqrt(jnp.mean(mixed * mixed, axis=-1, keepdims=True) + EPSILON) * norm_gain
    ).astype(bf16)
    return experts(
        normed, mixed, expert_ids, route_weight, expert_gate, expert_up, expert_down
    )


def solution(mesh):
    placed = (
        P("sp", "tp"),
        P("tp", None),
        P("tp", None),
        P(None, "tp", None, None),
        P("tp", None, None),
        P("tp"),
        P(),
        P(),
        P(("sp", "tp"), None),
        P(),
        P(("sp", "tp"), None),
        P(("sp", "tp"), None),
        P(("sp", "tp"), None, None),
        P(("sp", "tp"), None, None),
        P(("sp", "tp"), None, None),
    )
    return jax.shard_map(
        on_device, mesh=mesh, in_specs=placed, out_specs=P(("sp", "tp"), None), check_vma=False
    )
```

```python
import functools

import jax
import jax.numpy as jnp
from jax import lax
from jax.experimental import pallas as pl
from jax.experimental.pallas import tpu as pltpu
from jax.sharding import PartitionSpec as P

GROUPS = 4
EPSILON = 1e-06
LANES = 128
SEGMENTS = 8


def discretize(lam_real, lam_imag, state_in):
    magnitude = jnp.exp(lam_real)
    decay_re = magnitude * jnp.cos(lam_imag)
    decay_im = magnitude * jnp.sin(lam_imag)
    numer_re = decay_re - 1.0
    denom = lam_real * lam_real + lam_imag * lam_imag
    hold_re = ((numer_re * lam_real + decay_im * lam_imag) / denom)[:, None, :]
    hold_im = ((decay_im * lam_real - numer_re * lam_imag) / denom)[:, None, :]
    drive_re = hold_re * state_in[0] - hold_im * state_in[1]
    drive_im = hold_re * state_in[1] + hold_im * state_in[0]
    return drive_re.astype(jnp.bfloat16), drive_im.astype(jnp.bfloat16)


def powers(lam_real, lam_imag, exponent):
    magnitude = jnp.exp(exponent[:, None, None] * lam_real[None])
    angle = exponent[:, None, None] * lam_imag[None]
    return (magnitude * jnp.cos(angle), magnitude * jnp.sin(angle))


def iota(shape, dim):
    return lax.broadcasted_iota(jnp.int32, shape, dim)


def times(a_re, a_im, b_re, b_im):
    return a_re * b_re - a_im * b_im, a_re * b_im + a_im * b_re


def segment_order(rows, back=False):
    length = rows // SEGMENTS
    ordered, token = iota((rows, rows), 1 if back else 0), iota((rows, rows), 0 if back else 1)
    same = (ordered % SEGMENTS) * length + ordered // SEGMENTS == token
    return same.astype(jnp.float32).astype(jnp.bfloat16)


def spread(block, copies, row_group, column_group):
    rows, width = block.shape
    wide = width * copies
    pick = iota((width, wide), 0) == iota((width, wide), 1) % width
    tiled = jnp.dot(
        block, pick.astype(jnp.float32).astype(jnp.bfloat16), preferred_element_type=jnp.float32
    )
    keep = (iota((rows, wide), 0) // row_group) == (iota((rows, wide), 1) // column_group)
    return jnp.where(keep, tiled, 0.0).astype(jnp.bfloat16)


def ssm_ordered(x_ref):
    rows = x_ref.shape[0]
    return jnp.dot(
        segment_order(rows), x_ref[...], preferred_element_type=jnp.float32
    )


def fill_push(x_tile, drive_re_ref, drive_im_ref, tile, channels, push):
    states = drive_re_ref.shape[1]
    copies = LANES // channels
    width = copies * states
    rows = pl.ds(tile * LANES, LANES)
    for part, ref in enumerate((drive_re_ref, drive_im_ref)):
        block = spread(ref[rows, :], copies, channels, states)
        push[:, part * width : (part + 1) * width] = jnp.dot(
            x_tile, block, preferred_element_type=jnp.float32
        )


def run_scan(push, width, decay_re, decay_im, start_re, start_im, keep):
    shape = (SEGMENTS, width)
    decay_re = jnp.broadcast_to(decay_re, shape)
    decay_im = jnp.broadcast_to(decay_im, shape)

    def step(j, carry):
        rows = pl.ds(pl.multiple_of(j * SEGMENTS, SEGMENTS), SEGMENTS)
        next_re, next_im = times(decay_re, decay_im, *carry)
        next_re = next_re + push[rows, :width]
        next_im = next_im + push[rows, width:]
        if keep:
            push[rows, :width] = next_re
            push[rows, width:] = next_im
        return next_re, next_im

    return lax.fori_loop(0, push.shape[0] // SEGMENTS, step, (start_re, start_im), unroll=4)


MESH = pl.DeviceIdType.MESH


def mixer_kernel(channels, sp_count, x_ref, drive_re_ref, drive_im_ref, pow_re_ref, pow_im_ref,
                 read_ref, skip_ref, out_ref, push, start, pre, ends_re, ends_im, final, finals,
                 halves, taken, send_sem, recv_sem, swap_sem):
    mine, core = lax.axis_index("sp"), lax.axis_index("tp")

    def peer(step):
        return (lax.rem(mine + step, sp_count), core)

    barrier = pltpu.get_barrier_semaphore()

    @pl.loop(1, sp_count)
    def _(step):
        pl.semaphore_signal(barrier, inc=1, device_id=peer(step), device_id_type=MESH)

    pl.semaphore_signal(barrier, inc=1, device_id=(mine, 1 - core), device_id_type=MESH)

    wide = ssm_ordered(x_ref)
    ordered = wide.astype(jnp.bfloat16)
    rows = x_ref.shape[0]
    width = push.shape[2] // 2
    total = pow_re_ref.shape[1]
    states = drive_re_ref.shape[1]
    copies = LANES // channels
    for tile in range(total // width):
        lanes = slice(tile * width, (tile + 1) * width)
        fill_push(
            ordered[:, tile * LANES : (tile + 1) * LANES], drive_re_ref, drive_im_ref, tile,
            channels, push.at[tile],
        )
        zero = jnp.zeros((SEGMENTS, width), jnp.float32)
        end_re, end_im = run_scan(
            push.at[tile], width, pow_re_ref[0:1, lanes], pow_im_ref[0:1, lanes], zero, zero,
            False,
        )
        ends_re[:, lanes] = end_re
        ends_im[:, lanes] = end_im
        seg_re, seg_im = pow_re_ref[1:2, lanes], pow_im_ref[1:2, lanes]
        sum_re, sum_im = end_re[0:1], end_im[0:1]
        for s in range(1, SEGMENTS):
            sum_re, sum_im = times(seg_re, seg_im, sum_re, sum_im)
            sum_re, sum_im = sum_re + end_re[s : s + 1], sum_im + end_im[s : s + 1]
        final[0:1, lanes] = sum_re
        final[1:2, lanes] = sum_im

    pl.semaphore_wait(barrier, sp_count)

    def give(step):
        return pltpu.make_async_remote_copy(
            src_ref=final, dst_ref=finals.at[mine], send_sem=send_sem.at[step],
            recv_sem=recv_sem.at[step], device_id=peer(step), device_id_type=MESH,
        )

    @pl.loop(1, sp_count)
    def _(step):
        give(step).start()

    @pl.loop(1, sp_count)
    def _(step):
        give(step).wait()

    for tile in range(total // width):
        lanes = slice(tile * width, (tile + 1) * width)
        span_re, span_im = pow_re_ref[2:3, lanes], pow_im_ref[2:3, lanes]
        zero = jnp.zeros((1, width), jnp.float32)

        def hop(position, so_far):
            new_re, new_im = times(span_re, span_im, *so_far)
            return (new_re + finals[position, 0:1, lanes], new_im + finals[position, 1:2, lanes])

        in_re, in_im = lax.fori_loop(0, mine, hop, (zero, zero))
        seg_re, seg_im = pow_re_ref[1:2, lanes], pow_im_ref[1:2, lanes]
        for s in range(SEGMENTS):
            start[s : s + 1, :width] = in_re
            start[s : s + 1, width:] = in_im
            in_re, in_im = times(seg_re, seg_im, in_re, in_im)
            in_re = in_re + ends_re[s : s + 1, lanes]
            in_im = in_im + ends_im[s : s + 1, lanes]
        own = slice(tile * LANES, (tile + 1) * LANES)
        run_scan(
            push.at[tile], width, pow_re_ref[0:1, lanes], pow_im_ref[0:1, lanes],
            start[:, :width], start[:, width:], True,
        )
        read = jnp.zeros((rows, LANES), jnp.float32)
        for part in range(2):
            block = read_ref[tile * copies : (tile + 1) * copies,
                             part * states : (part + 1) * states, :]
            block = block.reshape(width, channels).astype(jnp.bfloat16)
            block = spread(block, copies, states, channels)
            read = read + jnp.dot(
                push[tile, :, part * width : (part + 1) * width].astype(jnp.bfloat16), block,
                preferred_element_type=jnp.float32,
            )
        value = jax.nn.gelu(read + skip_ref[0:1, own] * wide[:, own])
        pre[:, own] = value.astype(jnp.bfloat16)
    half = rows // 2
    back = jnp.dot(
        segment_order(rows, back=True), pre[...], preferred_element_type=jnp.float32
    ).astype(jnp.bfloat16)
    halves[0] = back[:half]
    halves[1] = back[half:]
    swap = pltpu.make_async_remote_copy(
        src_ref=halves.at[1 - core], dst_ref=taken, send_sem=swap_sem.at[0],
        recv_sem=swap_sem.at[1], device_id=(mine, 1 - core), device_id_type=MESH,
    )
    swap.start()
    wide_in = x_ref.shape[1]
    out_ref[:, pl.ds(pl.multiple_of(core * wide_in, LANES), wide_in)] = halves[core]
    swap.wait()
    out_ref[:, pl.ds(pl.multiple_of((1 - core) * wide_in, LANES), wide_in)] = taken[...]


def mixer(ssm_input, lam_real, lam_imag, state_in, read_out, channel_skip):
    rows, width_in = ssm_input.shape
    groups, states = lam_real.shape
    channels = state_in.shape[2]
    sp_count = lax.axis_size("sp")
    total = groups * states
    width = (LANES // channels) * states
    drive_re, drive_im = discretize(lam_real, lam_imag, state_in)
    drive_re = drive_re.reshape(width_in, states)
    drive_im = drive_im.reshape(width_in, states)
    steps = jnp.asarray([1.0, rows // SEGMENTS, rows], jnp.float32)
    pow_re, pow_im = powers(lam_real, lam_imag, steps)
    pow_re, pow_im = pow_re.reshape(3, total), pow_im.reshape(3, total)
    f32, bf16 = jnp.float32, jnp.bfloat16
    return pl.pallas_call(
        functools.partial(mixer_kernel, channels, sp_count),
        out_shape=jax.ShapeDtypeStruct((rows // 2, width_in * 2), bf16),
        scratch_shapes=[
            pltpu.VMEM((total // width, rows, 2 * width), f32),
            pltpu.VMEM((SEGMENTS, 2 * width), f32),
            pltpu.VMEM((rows, width_in), bf16),
            pltpu.VMEM((SEGMENTS, total), f32),
            pltpu.VMEM((SEGMENTS, total), f32),
            pltpu.VMEM((2, total), f32),
            pltpu.VMEM((sp_count, 2, total), f32),
            pltpu.VMEM((2, rows // 2, width_in), bf16),
            pltpu.VMEM((rows // 2, width_in), bf16),
            pltpu.SemaphoreType.DMA((sp_count,)),
            pltpu.SemaphoreType.DMA((sp_count,)),
            pltpu.SemaphoreType.DMA((2,)),
        ],
        compiler_params=pltpu.CompilerParams(collective_id=0, has_side_effects=True),
        name="mixer",
    )(ssm_input, drive_re, drive_im, pow_re, pow_im, read_out, channel_skip.reshape(1, width_in))


def place(meta, slots, weigh):
    tokens = meta.shape[1]
    slot = iota((slots, tokens), 0).astype(jnp.float32)
    total = jnp.zeros((slots, tokens), jnp.float32)
    for k in range(2):
        value = meta[2 + k : 3 + k] if weigh else 1.0
        total = total + jnp.where(slot == meta[k : k + 1], value, 0.0)
    return total


def experts_kernel(planes, members, cores, rows_ref, meta_ref, mixed_ref, gather_ref,
                   gate_hbm, up_hbm, down_hbm, out_ref, gate, up, down, got, got_meta, sent,
                   arrived, answer, back, joined, home, load_sem, z_send, z_recv, m_send, m_recv,
                   out_send, out_recv, ret_send, ret_recv, home_send, home_recv):
    f32, bf16 = jnp.float32, jnp.bfloat16
    loads = [
        pltpu.make_async_copy(hbm.at[0], vmem, load_sem.at[i])
        for i, (hbm, vmem) in enumerate(((gate_hbm, gate), (up_hbm, up), (down_hbm, down)))
    ]
    for load in loads:
        load.start()
    sp, core = lax.axis_index("sp"), lax.axis_index("tp")
    per_plane = members // cores
    plane = sp // per_plane
    column = sp - plane * per_plane
    member = column * cores + core

    def plane_at(step):
        return lax.rem(plane + step, planes)

    def above(step):
        return (plane_at(step) * per_plane + column, core)

    def member_at(step):
        return lax.rem(member + step, members)

    def beside(step):
        other = member_at(step)
        return (plane * per_plane + other // cores, lax.rem(other, cores))

    barrier = pltpu.get_barrier_semaphore()

    @pl.loop(1, planes)
    def _(step):
        pl.semaphore_signal(barrier, inc=1, device_id=above(step), device_id_type=MESH)

    @pl.loop(1, members)
    def _(step):
        pl.semaphore_signal(barrier, inc=1, device_id=beside(step), device_id_type=MESH)

    pl.semaphore_wait(barrier, planes + members - 2)

    def remote(src, dst, send, recv, where):
        return pltpu.make_async_remote_copy(
            src_ref=src, dst_ref=dst, send_sem=send, recv_sem=recv, device_id=where,
            device_id_type=MESH,
        )

    def meta_copy(d):
        return remote(meta_ref.at[plane_at(d)], got_meta.at[d], m_send.at[d], m_recv.at[d],
                      above(d))

    def rows_copy(d):
        return remote(rows_ref.at[plane_at(d)], got.at[d], z_send.at[d], z_recv.at[d], above(d))

    def out_copy(d, step):
        return remote(sent.at[d, member_at(step)], arrived.at[d, member], out_send.at[d, step],
                      out_recv.at[d, step], beside(step))

    def ret_copy(d, step):
        return remote(answer.at[d, member_at(step)], back.at[d, member], ret_send.at[d, step],
                      ret_recv.at[d, step], beside(step))

    def home_copy(d):
        return remote(joined.at[d], home.at[d], home_send.at[d], home_recv.at[d],
                      above(planes - d))

    for d in range(1, planes):
        meta_copy(d).start()
    for d in range(1, planes):
        rows_copy(d).start()

    capacity, model_width = sent.shape[2], sent.shape[3]
    slots = members * capacity
    tokens = rows_ref.shape[1]

    def dispatch(d):
        if d:
            meta_copy(d).wait_recv()
            rows_copy(d).wait_recv()
            block, meta = got[d], got_meta[d]
        else:
            block, meta = rows_ref[plane], meta_ref[plane]
        pick = place(meta[:, :tokens], slots, False).astype(bf16)
        spread_rows = jnp.dot(pick, block, preferred_element_type=f32).astype(bf16)
        sent[d] = spread_rows.reshape(members, capacity, model_width)

        @pl.loop(1, members)
        def _(step):
            out_copy(d, step).start()

        arrived[d, member] = sent[d, member]

    def expert(d):
        if d == 0:
            for load in loads:
                load.wait()

        @pl.loop(1, members)
        def _(step):
            out_copy(d, step).wait_recv()

        rows = arrived[d].reshape(slots, model_width)
        gate_part = jnp.dot(rows, gate[...], preferred_element_type=f32)
        up_part = jnp.dot(rows, up[...], preferred_element_type=f32)
        hidden = (jax.nn.silu(gate_part) * up_part).astype(bf16)
        result = jnp.dot(hidden, down[...], preferred_element_type=f32).astype(bf16)
        answer[d] = result.reshape(members, capacity, model_width)

        @pl.loop(1, members)
        def _(step):
            ret_copy(d, step).start()

        back[d, member] = answer[d, member]

    def join(d):
        @pl.loop(1, members)
        def _(step):
            ret_copy(d, step).wait_recv()

        meta = got_meta[d] if d else meta_ref[plane]
        weights = place(meta[:, :tokens], slots, True)
        coarse = weights.astype(bf16)
        fine = (weights - coarse.astype(f32)).astype(bf16)
        answers = back[d].reshape(slots, model_width)
        over_slots = (((0,), (0,)), ((), ()))
        total = lax.dot_general(coarse, answers, over_slots, preferred_element_type=f32)
        total = total + lax.dot_general(fine, answers, over_slots, preferred_element_type=f32)
        if d:
            joined[d] = total.astype(bf16)
            home_copy(d).start()
        else:
            home[0] = total.astype(bf16)

    for d in range(planes + 2):
        if d < planes:
            dispatch(d)
        if 1 <= d <= planes:
            expert(d - 1)
        if d >= 2:
            join(d - 2)

    total = mixed_ref[...]
    for d in range(planes):
        if d:
            home_copy(d).wait_recv()
        total = total + jnp.dot(
            gather_ref[plane_at(d)], home[d], preferred_element_type=f32
        )
    out_ref[...] = total.astype(bf16)

    for d in range(1, planes):
        meta_copy(d).wait_send()
        rows_copy(d).wait_send()
        home_copy(d).wait_send()

    for d in range(planes):
        @pl.loop(1, members)
        def _(step):
            out_copy(d, step).wait_send()
            ret_copy(d, step).wait_send()


def earlier_count(onehot):
    tokens = onehot.shape[0]
    earlier = (jnp.arange(tokens)[:, None] > jnp.arange(tokens)[None, :]).astype(jnp.bfloat16)
    return jnp.dot(earlier, onehot.astype(jnp.bfloat16), preferred_element_type=jnp.float32)


def routes(expert_ids, route_weight, members, capacity, room, padded):
    tokens = expert_ids.shape[0]
    count = members * GROUPS
    f32 = jnp.float32
    onehot = (expert_ids[:, :, None] == jnp.arange(count, dtype=jnp.int32)).astype(f32)
    both = jnp.sum(onehot, axis=1)
    group = expert_ids[:, 0] // members
    in_group = (group[:, None] == jnp.arange(GROUPS, dtype=jnp.int32)).astype(f32)
    before = earlier_count(jnp.concatenate([both, in_group], axis=1))
    rank = jnp.sum(before[:, None, :count] * onehot, axis=-1)
    slot = (expert_ids - group[:, None] * members).astype(f32) * padded + rank
    row = group * room + jnp.sum(before[:, count:] * in_group, axis=1).astype(jnp.int32)
    mine = row[None, :] == jnp.arange(GROUPS * room, dtype=jnp.int32)[:, None]
    values = jnp.concatenate([slot + 1.0, route_weight], axis=1)
    meta = jnp.sum(jnp.where(mine[None], values.T[:, None, :], 0.0), axis=-1)
    meta = meta - jnp.asarray([1.0, 1.0, 0.0, 0.0], f32)[:, None]
    meta = meta.reshape(4, GROUPS, room).transpose(1, 0, 2)
    meta = jnp.pad(meta, ((0, 0), (0, 4), (0, -room % LANES)))
    return mine.astype(jnp.bfloat16), meta


def experts(normed, mixed, expert_ids, route_weight, expert_gate, expert_up, expert_down):
    f32, bf16 = jnp.float32, jnp.bfloat16
    tokens, model_width = normed.shape
    hidden = expert_gate.shape[2]
    cores = lax.axis_size("tp")
    members = lax.axis_size("sp") * cores // GROUPS
    capacity = tokens // members
    room = members * capacity // expert_ids.shape[1]
    padded = -(-capacity // 16) * 16
    mine, meta = routes(expert_ids, route_weight, members, capacity, room, padded)
    rows = jnp.dot(mine, normed, preferred_element_type=f32).astype(bf16)
    rows = rows.reshape(GROUPS, room, model_width)
    gather = mine.reshape(GROUPS, room, tokens).transpose(0, 2, 1)
    vmem = pl.BlockSpec(memory_space=pltpu.VMEM)
    hbm = pl.BlockSpec(memory_space=pl.ANY)
    block = pltpu.VMEM((GROUPS, members, padded, model_width), bf16)
    group_rows = pltpu.VMEM((GROUPS, room, model_width), bf16)
    dma = pltpu.SemaphoreType.DMA
    return pl.pallas_call(
        functools.partial(experts_kernel, GROUPS, members, cores),
        out_shape=jax.ShapeDtypeStruct((tokens, model_width), bf16),
        in_specs=[vmem] * 4 + [hbm] * 3,
        out_specs=vmem,
        scratch_shapes=[
            pltpu.VMEM((model_width, hidden), bf16),
            pltpu.VMEM((model_width, hidden), bf16),
            pltpu.VMEM((hidden, model_width), bf16),
            group_rows,
            pltpu.VMEM(meta.shape, f32),
            block, block, block, block,
            group_rows, group_rows,
            dma((3,)),
            dma((GROUPS,)), dma((GROUPS,)), dma((GROUPS,)), dma((GROUPS,)),
            dma((GROUPS, members)), dma((GROUPS, members)),
            dma((GROUPS, members)), dma((GROUPS, members)),
            dma((GROUPS,)), dma((GROUPS,)),
        ],
        compiler_params=pltpu.CompilerParams(collective_id=1, has_side_effects=True),
        name="experts",
    )(rows, meta, mixed, gather, expert_gate, expert_up, expert_down)


def on_device(
    ssm_input,
    lam_real,
    lam_imag,
    state_in,
    read_out,
    channel_skip,
    glu_weight,
    out_weight,
    residual,
    norm_gain,
    expert_ids,
    route_weight,
    expert_gate,
    expert_up,
    expert_down,
):
    f32, bf16 = jnp.float32, jnp.bfloat16
    own_tokens = mixer(ssm_input, lam_real, lam_imag, state_in, read_out, channel_skip)
    gate_lin = jnp.dot(own_tokens, glu_weight, preferred_element_type=f32)
    gated = (own_tokens.astype(f32) * jax.nn.sigmoid(gate_lin)).astype(bf16)
    mixed = residual.astype(f32) + jnp.dot(gated, out_weight, preferred_element_type=f32)
    normed = (
        mixed * lax.rsqrt(jnp.mean(mixed * mixed, axis=-1, keepdims=True) + EPSILON) * norm_gain
    ).astype(bf16)
    return experts(
        normed, mixed, expert_ids, route_weight, expert_gate, expert_up, expert_down
    )


def solution(mesh):
    placed = (
        P("sp", "tp"),
        P("tp", None),
        P("tp", None),
        P(None, "tp", None, None),
        P("tp", None, None),
        P("tp"),
        P(),
        P(),
        P(("sp", "tp"), None),
        P(),
        P(("sp", "tp"), None),
        P(("sp", "tp"), None),
        P(("sp", "tp"), None, None),
        P(("sp", "tp"), None, None),
        P(("sp", "tp"), None, None),
    )
    return jax.shard_map(
        on_device, mesh=mesh, in_specs=placed, out_specs=P(("sp", "tp"), None), check_vma=False
    )
```
